32 devices in a mesh: grp: 2 (over y), sp: 4 (over z), tp: 4 (over x, core).
Axes of the slice: x: 2, y: 2, z: 4, core: 2. Of those that a mesh axis runs over, the one named last changes fastest.
Arguments:
- queries_small: bfloat16 [2048, 1024], P(('grp', 'sp'), 'tp'), parts along dimension 0, may hold values from -6 to 6
- keys_small: bfloat16 [2048, 512], P(('grp', 'sp'), 'tp'), parts along dimension 0, may hold values from -6 to 6
- values_small: bfloat16 [2048, 512], P(('grp', 'sp'), 'tp'), parts along dimension 0, may hold values from -6 to 6
- queries_large: bfloat16 [2048, 1024], P(('grp', 'sp'), 'tp'), parts along dimension 0, may hold values from -6 to 6
- keys_large: bfloat16 [2048, 512], P(('grp', 'sp'), 'tp'), parts along dimension 0, may hold values from -6 to 6
- values_large: bfloat16 [2048, 512], P(('grp', 'sp'), 'tp'), parts along dimension 0, may hold values from -6 to 6
- query_gain_small: float32 [128], P('grp'), parts along dimension 0, may hold values from 1.2 to 12
- key_gain_small: float32 [128], P('grp'), parts along dimension 0, may hold values from 1.2 to 12
- query_gain_large: float32 [256], P('grp'), parts along dimension 0, may hold values from 1.2 to 12
- key_gain_large: float32 [256], P('grp'), parts along dimension 0, may hold values from 1.2 to 12
- residual_in: bfloat16 [2048, 2048], P(('grp', 'sp', 'tp')), parts along dimension 0, may hold values from -1.5 to 1.5
- out_weight_small: bfloat16 [1024, 2048], P('tp'), may hold values from -0.125 to 0.125
- out_weight_large: bfloat16 [1024, 2048], P('tp'), may hold values from -0.125 to 0.125
- norm_gain: float32 [2048], replicated, may hold values from 0.1 to 1.9
- routes: int32 [2048, 2], P(('grp', 'sp', 'tp')), parts along dimension 0, may hold values from 0 to 7, all different within a row; in each aligned block of 64 rows (0 to 63, 64 to 127, ...) at most 32 rows name the same one
- route_scores: float32 [2048, 2], P(('grp', 'sp', 'tp')), parts along dimension 0, may hold values from 0.05 to 1
- expert_gate: bfloat16 [8, 2048, 1024], P('sp', None, 'tp'), may hold values from -0.125 to 0.125
- expert_up: bfloat16 [8, 2048, 1024], P('sp', None, 'tp'), may hold values from -0.125 to 0.125
- expert_down: bfloat16 [8, 1024, 2048], P('sp', 'tp'), may hold values from -0.1875 to 0.1875
Outputs:
- result: bfloat16 [2048, 2048], P(('grp', 'sp', 'tp')), parts along dimension 0
The draws below stay inside these ranges and needn't reach their ends.
There are 2 independent parts, one for each index of `grp`. The reference program is written for one: setup_inputs(seed, part) draws one part's arguments, and reference() takes and returns one part's arrays. A program takes and returns all parts, laid end to end along the dimension named above; an argument that names none is the same for every part. Nothing has to cross between parts.
Inputs may be any that keep to these rules, and one draw needn't show every extreme that they name: `routes`: each token names 2 different experts; within the rows of one device (aligned blocks of 64 tokens) no expert is named more than 32 times, a bound that some block reaches.
All inputs are finite; a program needn't handle non-finite values.
Results may differ from the reference program's by a relative error of at most 0.02.
The reference program's roundings to bfloat16 on the way count: a program that leaves them out, or rounds other values in their place, can miss the bound.
Values may be sent and summed in bfloat16 or wider, within the bound.
No kernel may reach another device: no remote copies, remote signals or barrier semaphores. Data moves between devices by JAX's collectives and lax.ppermute only.
A program may use at most 128 MiB of HBM per device.

```python
import math
import jax
import jax.numpy as jnp
import numpy as np
from jax import lax

D = 2048
FFE = 1024
HS_SMALL = 64
HS_LARGE = 128
Q_SMALL = 16
KV_SMALL = 8
Q_LARGE = 8
KV_LARGE = 4
GRID_W = 64
TOP = 2
TOK_DEV = 256
SEQ = 1024
ROWS_DEV = 64
EXPERTS = 8
CAP = 32
N_TP = 4


def group_draw(key, query_heads, key_heads, head_size):
    draw_keys = jax.random.split(jax.random.fold_in(key, 7919 + head_size), 4)
    key_rows = jnp.clip(jax.random.normal(draw_keys[0], (SEQ, key_heads * head_size), jnp.float32), -6.0, 6.0)
    query_rows = jnp.clip(jax.random.normal(draw_keys[1], (SEQ, query_heads * head_size), jnp.float32), -6.0, 6.0)
    query_gain = jax.random.uniform(draw_keys[2], (head_size,), jnp.float32, 1.2, 2.0)
    key_gain = jax.random.uniform(draw_keys[3], (head_size,), jnp.float32, 1.2, 2.0)
    return (query_rows, key_rows, query_gain, key_gain)


def draw_queries_small(key, part):
    return group_draw(key, Q_SMALL, KV_SMALL, HS_SMALL)[0].astype(jnp.bfloat16)


def draw_keys_small(key, part):
    return group_draw(key, Q_SMALL, KV_SMALL, HS_SMALL)[1].astype(jnp.bfloat16)


def draw_query_gain_small(key, part):
    return group_draw(key, Q_SMALL, KV_SMALL, HS_SMALL)[2].astype(jnp.float32)


def draw_key_gain_small(key, part):
    return group_draw(key, Q_SMALL, KV_SMALL, HS_SMALL)[3].astype(jnp.float32)


def draw_queries_large(key, part):
    return group_draw(key, Q_LARGE, KV_LARGE, HS_LARGE)[0].astype(jnp.bfloat16)


def draw_keys_large(key, part):
    return group_draw(key, Q_LARGE, KV_LARGE, HS_LARGE)[1].astype(jnp.bfloat16)


def draw_query_gain_large(key, part):
    return group_draw(key, Q_LARGE, KV_LARGE, HS_LARGE)[2].astype(jnp.float32)


def draw_key_gain_large(key, part):
    return group_draw(key, Q_LARGE, KV_LARGE, HS_LARGE)[3].astype(jnp.float32)


def shard_levels(key, shape, pieces, low, largest):
    def one(axis_at, blocks):
        steps = jax.random.uniform(jax.random.fold_in(jax.random.fold_in(key, 6), axis_at), (blocks,), jnp.float32, low / len(pieces), largest / len(pieces))
        return jnp.repeat(jnp.exp(steps), shape[axis_at] // blocks).reshape((-1,) + (1,) * (len(shape) - axis_at - 1))

    loudness = one(*pieces[0])
    for cut in pieces[1:]:
        loudness = loudness * one(*cut)
    return loudness


def deal_out(own_key, own, number, rows, count, top, reach, slope):
    ranking = jax.random.permutation(own_key, count)
    crowded, usual = portions_of(count, rows * top, reach, slope, True), portions_of(count, rows * top, reach, slope, False)
    places = jnp.arange(count)

    def named(lengths, offset_by):
        used = int((lengths > 0).sum())
        fixed = max(1, used // 4)
        passed = fixed + (places - fixed + offset_by * (used - fixed)) % max(1, count - fixed)
        return jnp.zeros((count,), jnp.int32).at[ranking[jnp.where(places < fixed, places, passed)]].set(jnp.asarray(lengths, jnp.int32))

    lengths = jnp.where(number % 4 == 0, named(crowded, number // 4), named(usual, number - number // 4 - 1))
    mixed = jax.random.permutation(jax.random.fold_in(own, 3), count)
    giver, sink = mixed[0:count // 2 * 2:2], mixed[1:count // 2 * 2:2]
    slack = jnp.minimum(lengths[giver] - 1, reach - lengths[sink]) // 2
    slack = jnp.where((giver == ranking[0]) | (sink == ranking[0]) | (lengths[sink] == 0), 0, jnp.maximum(slack, 0))
    passed = jax.random.randint(jax.random.fold_in(own, 4), (count // 2,), 0, 1 << 20) % (slack + 1)
    lengths = lengths.at[giver].add(-passed).at[sink].add(passed)
    members = jnp.searchsorted(jnp.cumsum(lengths), jnp.arange(rows * top), side="right").astype(jnp.int32)
    listing = members.reshape(top, rows).T
    listing = listing[jax.random.permutation(jax.random.fold_in(own, 1), rows)]
    offset_by = jax.random.randint(jax.random.fold_in(own, 2), (rows, 1), 0, top)
    return jnp.take_along_axis(listing, (jnp.arange(top)[None, :] + offset_by) % top, axis=1)


def portions_of(amount, total, reach, skew, full):
    weights = [(1 << 20) // math.isqrt(standing ** skew) + 1 for standing in range(1, amount + 1)]
    largest = reach if full else min(reach, max(-(-total // amount), total * weights[0] // sum(weights)))
    least = 1 if total - largest >= amount - 1 else 0
    given, surplus = [largest] + [least] * (amount - 1), total - largest - least * (amount - 1)
    while surplus > 0:
        movable = [i for i in range(1, amount) if given[i] < largest] or [i for i in range(1, amount) if given[i] < reach]
        mass, remaining = sum([weights[i] for i in movable]), surplus
        for i in movable:
            addition = min(reach - given[i], max(1, remaining * weights[i] // mass), surplus)
            given[i] = given[i] + addition
            surplus = surplus - addition
    return np.array(given)


def normal_values(key, extent, scale, most, cuts=(), held_as=jnp.bfloat16):
    factor_of = shard_levels(key, extent, cuts, -0.22, 0.18) if cuts else 1.0
    array = jax.random.normal(key, extent, jnp.float32) * scale * factor_of
    return jnp.minimum(jnp.maximum(array, -most), most).astype(held_as)


def setup_inputs(seed: int = 0, part: int = 0) -> dict:
    keys = jax.random.split(jax.random.key(seed), 20)
    part_keys = jax.random.split(jax.random.fold_in(keys[19], part), 20)
    queries_small = draw_queries_small(jax.random.fold_in(jax.random.fold_in(keys[19], part), 71), part)
    keys_small = draw_keys_small(jax.random.fold_in(jax.random.fold_in(keys[19], part), 71), part)
    values_small = normal_values(part_keys[2], (SEQ, KV_SMALL * HS_SMALL), 1.0, 6.0, ((0, 4), (1, 4)))
    queries_large = draw_queries_large(jax.random.fold_in(jax.random.fold_in(keys[19], part), 71), part)
    keys_large = draw_keys_large(jax.random.fold_in(jax.random.fold_in(keys[19], part), 71), part)
    values_large = normal_values(part_keys[5], (SEQ, KV_LARGE * HS_LARGE), 1.0, 6.0, ((0, 4), (1, 4)))
    query_gain_small = draw_query_gain_small(jax.random.fold_in(jax.random.fold_in(keys[19], part), 71), part)
    key_gain_small = draw_key_gain_small(jax.random.fold_in(jax.random.fold_in(keys[19], part), 71), part)
    query_gain_large = draw_query_gain_large(jax.random.fold_in(jax.random.fold_in(keys[19], part), 71), part)
    key_gain_large = draw_key_gain_large(jax.random.fold_in(jax.random.fold_in(keys[19], part), 71), part)
    residual_in = normal_values(part_keys[10], (SEQ, D), 0.25, 1.5, ((0, 16),))
    out_weight_small = normal_values(keys[11], (Q_SMALL * HS_SMALL, D), (Q_SMALL * HS_SMALL + Q_LARGE * HS_LARGE) ** -0.5, 0.125, ((0, 4),))
    out_weight_large = normal_values(keys[12], (Q_LARGE * HS_LARGE, D), (Q_SMALL * HS_SMALL + Q_LARGE * HS_LARGE) ** -0.5, 0.125, ((0, 4),))
    norm_gain = jnp.clip(1.0 + 0.18 * jax.random.normal(keys[13], (D,), jnp.float32), 0.1, 1.9)
    routes_keys = jax.random.split(jax.random.fold_in(part_keys[14], 1), SEQ // ROWS_DEV)
    routes_turns = jax.random.permutation(jax.random.fold_in(part_keys[14], 3), SEQ // ROWS_DEV)
    routes = jax.vmap(lambda own, number: deal_out(jax.random.fold_in(part_keys[14], 2), own, number, ROWS_DEV, EXPERTS, TOP, CAP, 1))(routes_keys, routes_turns).reshape((SEQ, TOP))
    route_scores = jnp.clip(0.05 + 0.95 * jax.random.uniform(part_keys[15], (SEQ, TOP), jnp.float32) ** shard_levels(part_keys[15], (SEQ, TOP), ((0, 16),), -0.2, 0.2), 0.05, 1.0)
    expert_gate = normal_values(keys[16], (EXPERTS, D, FFE), D ** -0.5, 0.125, ((0, 4), (2, 4)))
    expert_up = normal_values(keys[17], (EXPERTS, D, FFE), D ** -0.5, 0.125, ((0, 4), (2, 4)))
    expert_down = normal_values(keys[18], (EXPERTS, FFE, D), FFE ** -0.5, 0.1875, ((0, 4), (1, 4)))
    return dict(queries_small=queries_small, keys_small=keys_small, values_small=values_small, queries_large=queries_large, keys_large=keys_large, values_large=values_large, query_gain_small=query_gain_small, key_gain_small=key_gain_small, query_gain_large=query_gain_large, key_gain_large=key_gain_large, residual_in=residual_in, out_weight_small=out_weight_small, out_weight_large=out_weight_large, norm_gain=norm_gain, routes=routes, route_scores=route_scores, expert_gate=expert_gate, expert_up=expert_up, expert_down=expert_down)


theta_base = 10000.0
norm_eps = 1e-06

def grid_tables(offset, length, head_size):
    places = offset + jnp.arange(length, dtype=jnp.int32)
    grid_rows = (places // GRID_W).astype(jnp.float32)
    grid_cols = (places % GRID_W).astype(jnp.float32)
    rates = jnp.power(theta_base, -2.0 * jnp.arange(head_size // 4, dtype=jnp.float32) / (head_size // 2))
    row_angles = grid_rows[:, None, None] * rates
    col_angles = grid_cols[:, None, None] * rates
    return (jnp.cos(row_angles), jnp.sin(row_angles), jnp.cos(col_angles), jnp.sin(col_angles))

def half_turn(segment, cosine, sine_part):
    half_size = segment.shape[-1] // 2
    leading = segment[..., :half_size]
    trailing = segment[..., half_size:]
    return jnp.concatenate([leading * cosine - trailing * sine_part, trailing * cosine + leading * sine_part], axis=-1)

def grid_turn(vectors, tables):
    row_cos, row_sin, col_cos, col_sin = tables
    half_size = vectors.shape[-1] // 2
    return jnp.concatenate([half_turn(vectors[..., :half_size], row_cos, row_sin), half_turn(vectors[..., half_size:], col_cos, col_sin)], axis=-1)

def normed_turn(raw_rows, gain, tables):
    widened = raw_rows.astype(jnp.float32)
    scaled = widened * lax.rsqrt(lax.optimization_barrier(jnp.mean(widened * widened, axis=-1, keepdims=True)) + norm_eps) * gain
    return grid_turn(scaled, tables).astype(jnp.bfloat16)

def attend_group(queries, key_rows, value_rows, query_gain, key_gain, head_size):
    seq_len = queries.shape[0]
    query_heads = queries.shape[1] // head_size
    key_heads = key_rows.shape[1] // head_size
    group_ratio = query_heads // key_heads
    tables = grid_tables(0, seq_len, head_size)
    asked = normed_turn(queries.reshape(seq_len, query_heads, head_size), query_gain, tables)
    keyed = normed_turn(key_rows.reshape(seq_len, key_heads, head_size), key_gain, tables)
    valued = value_rows.reshape(seq_len, key_heads, head_size)

    def one_head(head_index):
        asked_head = lax.dynamic_index_in_dim(asked, head_index, 1, keepdims=False)
        keyed_head = lax.dynamic_index_in_dim(keyed, head_index // group_ratio, 1, keepdims=False)
        valued_head = lax.dynamic_index_in_dim(valued, head_index // group_ratio, 1, keepdims=False)

        def one_block(query_block):
            scores = jnp.dot(query_block, keyed_head.T, preferred_element_type=jnp.float32) * head_size ** (-0.5)
            peak_score = lax.optimization_barrier(jnp.max(scores, axis=1, keepdims=True))
            weights = jnp.exp(scores - peak_score)
            summed = jnp.dot(weights.astype(jnp.bfloat16), valued_head, preferred_element_type=jnp.float32)
            return (summed / lax.optimization_barrier(jnp.sum(weights, axis=1, keepdims=True))).astype(jnp.bfloat16)
        blocks = asked_head.reshape(seq_len // TOK_DEV, TOK_DEV, head_size)
        return lax.map(one_block, blocks).reshape(seq_len, head_size)
    heard = lax.map(one_head, jnp.arange(query_heads, dtype=jnp.int32))
    return jnp.transpose(heard, (1, 0, 2)).reshape(seq_len, query_heads * head_size)

def expert_chain(rows_in, gate_weight, up_weight, down_weight):
    gate_out = jnp.dot(rows_in, gate_weight, preferred_element_type=jnp.float32)
    up_out = jnp.dot(rows_in, up_weight, preferred_element_type=jnp.float32)
    active = (jax.nn.silu(gate_out) * up_out).astype(jnp.bfloat16)
    width_part = FFE // N_TP
    total_terms = jnp.zeros((rows_in.shape[0], D), jnp.float32)
    for part_index in range(N_TP):
        lower = part_index * width_part
        term = jnp.dot(active[:, lower:lower + width_part], down_weight[lower:lower + width_part], preferred_element_type=jnp.float32).astype(jnp.bfloat16)
        total_terms = total_terms + lax.optimization_barrier(term).astype(jnp.float32)
    return total_terms.astype(jnp.bfloat16)

def reference(queries_small, keys_small, values_small, queries_large, keys_large, values_large, query_gain_small, key_gain_small, query_gain_large, key_gain_large, residual_in, out_weight_small, out_weight_large, norm_gain, routes, route_scores, expert_gate, expert_up, expert_down):
    heard_small = attend_group(queries_small, keys_small, values_small, query_gain_small, key_gain_small, HS_SMALL)
    heard_large = attend_group(queries_large, keys_large, values_large, query_gain_large, key_gain_large, HS_LARGE)
    small_cols = Q_SMALL * HS_SMALL // N_TP
    large_cols = Q_LARGE * HS_LARGE // N_TP
    projected = jnp.zeros((SEQ, D), jnp.float32)
    for part_index in range(N_TP):
        lower_small = part_index * small_cols
        lower_large = part_index * large_cols
        term = jnp.dot(heard_small[:, lower_small:lower_small + small_cols], out_weight_small[lower_small:lower_small + small_cols], preferred_element_type=jnp.float32) + jnp.dot(heard_large[:, lower_large:lower_large + large_cols], out_weight_large[lower_large:lower_large + large_cols], preferred_element_type=jnp.float32)
        term = term.astype(jnp.bfloat16)
        projected = projected + lax.optimization_barrier(term).astype(jnp.float32)
    attended = (residual_in.astype(jnp.float32) + projected).astype(jnp.bfloat16)
    widened = attended.astype(jnp.float32)
    normed = (widened * lax.rsqrt(lax.optimization_barrier(jnp.mean(widened * widened, axis=-1, keepdims=True)) + norm_eps) * norm_gain).astype(jnp.bfloat16)
    shares = route_scores / lax.optimization_barrier(jnp.sum(route_scores, axis=1, keepdims=True))
    block_count = SEQ // ROWS_DEV
    flat_routes = routes.reshape(block_count, ROWS_DEV * TOP)
    member = (flat_routes[:, :, None] == jnp.arange(EXPERTS, dtype=jnp.int32)[None, None, :]).astype(jnp.int32)
    ranks = lax.optimization_barrier(jnp.sum((jnp.cumsum(member, axis=1) - member) * member, axis=2))
    slot_within = jnp.arange(block_count, dtype=jnp.int32)[:, None] * CAP + ranks
    token_ids = jnp.arange(SEQ, dtype=jnp.int32).reshape(block_count, ROWS_DEV)
    token_of = jnp.broadcast_to(token_ids[:, :, None], (block_count, ROWS_DEV, TOP)).reshape(-1)
    slot_tokens = jnp.zeros((EXPERTS, block_count * CAP), jnp.int32).at[flat_routes.reshape(-1), slot_within.reshape(-1)].set(token_of)
    slot_shares = jnp.zeros((EXPERTS, block_count * CAP), jnp.float32).at[flat_routes.reshape(-1), slot_within.reshape(-1)].set(shares.reshape(-1))

    def add_expert(mixed, inputs):
        tokens_here, shares_here, gate_weight, up_weight, down_weight = inputs
        outputs = expert_chain(normed[tokens_here], gate_weight, up_weight, down_weight)
        return (mixed.at[tokens_here].add(outputs.astype(jnp.float32) * shares_here[:, None]), None)
    mixed = lax.scan(add_expert, jnp.zeros((SEQ, D), jnp.float32), (slot_tokens, slot_shares, expert_gate, expert_up, expert_down))[0]
    return (attended.astype(jnp.float32) + mixed).astype(jnp.bfloat16)
```

```python
import jax
import jax.numpy as jnp
from jax import lax
from jax.sharding import PartitionSpec as P

HS_SMALL = 64
HS_LARGE = 128
GRID_W = 64


theta_base = 10000.0
norm_eps = 1e-06
block_target = 1280


def grid_tables(offset, length, head_size):
    places = offset + jnp.arange(length, dtype=jnp.int32)
    grid_rows = (places // GRID_W).astype(jnp.float32)
    grid_cols = (places % GRID_W).astype(jnp.float32)
    rates = jnp.power(
        theta_base, -2.0 * jnp.arange(head_size // 4, dtype=jnp.float32) / (head_size // 2)
    )
    row_angles = grid_rows[:, None, None] * rates
    col_angles = grid_cols[:, None, None] * rates
    return (jnp.cos(row_angles), jnp.sin(row_angles), jnp.cos(col_angles), jnp.sin(col_angles))


def half_turn(segment, cosine, sine_part):
    half_size = segment.shape[-1] // 2
    leading = segment[..., :half_size]
    trailing = segment[..., half_size:]
    return jnp.concatenate(
        [leading * cosine - trailing * sine_part, trailing * cosine + leading * sine_part], axis=-1
    )


def grid_turn(vectors, tables):
    row_cos, row_sin, col_cos, col_sin = tables
    half_size = vectors.shape[-1] // 2
    return jnp.concatenate(
        [
            half_turn(vectors[..., :half_size], row_cos, row_sin),
            half_turn(vectors[..., half_size:], col_cos, col_sin),
        ],
        axis=-1,
    )


def normed_turn(raw_rows, gain, tables):
    widened = raw_rows.astype(jnp.float32)
    scaled = (
        widened * lax.rsqrt(jnp.mean(widened * widened, axis=-1, keepdims=True) + norm_eps) * gain
    )
    return grid_turn(scaled, tables).astype(jnp.bfloat16)


def block_rows(row_count, shard_rows):
    shards = row_count // shard_rows
    chosen = 1
    for factor in range(1, max(1, block_target // shard_rows) + 1):
        if shards % factor == 0:
            chosen = factor
    return chosen * shard_rows


def attend_block(state, queries, key_rows, value_rows):
    largest, weight_sum, accumulated = state
    head_size = queries.shape[-1]
    kv_local = queries.shape[1]
    key_heads = key_rows.reshape(key_rows.shape[0], kv_local, head_size)
    value_heads = value_rows.reshape(value_rows.shape[0], kv_local, head_size)
    scores = jnp.einsum(
        "qgrd,kgd->qgrk", queries, key_heads, preferred_element_type=jnp.float32
    ) * head_size ** (-0.5)
    peak_score = jnp.maximum(largest, jnp.max(scores, axis=-1))
    shrink = jnp.exp(largest - peak_score)
    weights = jnp.exp(scores - peak_score[..., None])
    weight_sum = weight_sum * shrink + jnp.sum(weights, axis=-1)
    accumulated = accumulated * shrink[..., None] + jnp.einsum(
        "qgrk,kgd->qgrd",
        weights.astype(jnp.bfloat16),
        value_heads,
        preferred_element_type=jnp.float32,
    )
    return (peak_score, weight_sum, accumulated)


def attend_rows(state, queries, key_rows, value_rows):
    row_count = key_rows.shape[0]
    step_rows = block_rows(row_count, queries.shape[0])
    if step_rows == row_count:
        return attend_block(state, queries, key_rows, value_rows)

    def one_block(block_index, carried):
        offset = block_index * step_rows
        return attend_block(
            carried,
            queries,
            lax.dynamic_slice_in_dim(key_rows, offset, step_rows, 0),
            lax.dynamic_slice_in_dim(value_rows, offset, step_rows, 0),
        )

    return lax.fori_loop(0, row_count // step_rows, one_block, state)


def empty_state(queries):
    state_shape = queries.shape[:3]
    return (
        jnp.full(state_shape, -1e30, jnp.float32),
        jnp.zeros(state_shape, jnp.float32),
        jnp.zeros(queries.shape, jnp.float32),
    )


def finish(state):
    largest, weight_sum, accumulated = state
    merged = accumulated / weight_sum[..., None]
    return merged.reshape(merged.shape[0], -1).astype(jnp.bfloat16)


def dispatch_plan(
    queries_small,
    keys_small,
    values_small,
    queries_large,
    keys_large,
    values_large,
    query_gain_small,
    key_gain_small,
    query_gain_large,
    key_gain_large,
    residual_in,
    out_weight_small,
    out_weight_large,
    norm_gain,
    routes,
    route_scores,
    expert_gate,
    expert_up,
    expert_down,
):
    token_rows = queries_small.shape[0]
    offset = lax.axis_index("sp") * token_rows
    tables_small = grid_tables(offset, token_rows, HS_SMALL)
    tables_large = grid_tables(offset, token_rows, HS_LARGE)
    kv_small = keys_small.shape[1] // HS_SMALL
    kv_large = keys_large.shape[1] // HS_LARGE
    asked_small = normed_turn(
        queries_small.reshape(token_rows, -1, HS_SMALL), query_gain_small, tables_small
    ).reshape(token_rows, kv_small, -1, HS_SMALL)
    asked_large = normed_turn(
        queries_large.reshape(token_rows, -1, HS_LARGE), query_gain_large, tables_large
    ).reshape(token_rows, kv_large, -1, HS_LARGE)
    turned_small = normed_turn(
        keys_small.reshape(token_rows, kv_small, HS_SMALL), key_gain_small, tables_small
    ).reshape(token_rows, -1)
    turned_large = normed_turn(
        keys_large.reshape(token_rows, kv_large, HS_LARGE), key_gain_large, tables_large
    ).reshape(token_rows, -1)
    key_small = lax.all_gather(turned_small, "sp", axis=0, tiled=True)
    value_small = lax.all_gather(values_small, "sp", axis=0, tiled=True)
    key_large = lax.all_gather(turned_large, "sp", axis=0, tiled=True)
    value_large = lax.all_gather(values_large, "sp", axis=0, tiled=True)
    state_small = attend_rows(empty_state(asked_small), asked_small, key_small, value_small)
    state_large = attend_rows(empty_state(asked_large), asked_large, key_large, value_large)
    heard_small = finish(state_small)
    heard_large = finish(state_large)
    projected = lax.psum_scatter(
        (
            jnp.dot(heard_small, out_weight_small, preferred_element_type=jnp.float32)
            + jnp.dot(heard_large, out_weight_large, preferred_element_type=jnp.float32)
        ).astype(jnp.bfloat16),
        "tp",
        scatter_dimension=0,
        tiled=True,
    ).astype(jnp.float32)
    attended = (residual_in.astype(jnp.float32) + projected).astype(jnp.bfloat16)
    widened = attended.astype(jnp.float32)
    normed = (
        widened
        * lax.rsqrt(jnp.mean(widened * widened, axis=-1, keepdims=True) + norm_eps)
        * norm_gain
    ).astype(jnp.bfloat16)
    local_rows = routes.shape[0]
    top_count = routes.shape[1]
    sp_count = lax.axis_size("sp")
    local_experts = expert_gate.shape[0]
    expert_count = local_experts * sp_count
    capacity = max(2, (2 * top_count * local_rows + expert_count - 1) // expert_count)
    flat_routes = routes.reshape(-1)
    member = (flat_routes[:, None] == jnp.arange(expert_count, dtype=jnp.int32)[None, :]).astype(
        jnp.int32
    )
    ranks = jnp.sum((jnp.cumsum(member, axis=0) - member) * member, axis=1)
    slots = flat_routes * capacity + ranks
    picker = (
        slots[:, None] == jnp.arange(expert_count * capacity, dtype=jnp.int32)[None, :]
    ).astype(jnp.bfloat16)
    placer = jnp.sum(picker.reshape(local_rows, top_count, -1), axis=1)
    outgoing = jnp.einsum("ts,td->sd", placer, normed, preferred_element_type=jnp.float32).astype(
        jnp.bfloat16
    )
    outgoing = outgoing.reshape(sp_count, local_experts, capacity, -1)
    everyone = lax.all_gather(
        lax.all_to_all(outgoing, "sp", split_axis=0, concat_axis=0, tiled=True),
        "tp",
        axis=0,
        tiled=True,
    )
    gate_out = jnp.einsum(
        "secd,edf->secf", everyone, expert_gate, preferred_element_type=jnp.float32
    )
    up_out = jnp.einsum("secd,edf->secf", everyone, expert_up, preferred_element_type=jnp.float32)
    active = (jax.nn.silu(gate_out) * up_out).astype(jnp.bfloat16)
    summed = lax.psum_scatter(
        jnp.einsum(
            "secf,efd->secd", active, expert_down, preferred_element_type=jnp.float32
        ).astype(jnp.bfloat16),
        "tp",
        scatter_dimension=0,
        tiled=True,
    )
    returned = lax.all_to_all(summed, "sp", split_axis=0, concat_axis=0, tiled=True)
    back_rows = returned.reshape(expert_count * capacity, -1)
    chosen_rows = jnp.dot(picker, back_rows, preferred_element_type=jnp.float32).reshape(
        local_rows, top_count, -1
    )
    shares = route_scores / jnp.sum(route_scores, axis=1, keepdims=True)
    mixed = jnp.sum(chosen_rows * shares[:, :, None], axis=1)
    return (attended.astype(jnp.float32) + mixed).astype(jnp.bfloat16)


def swap(values, axis, flip):
    size = lax.axis_size(axis)
    return lax.ppermute(values, axis, [(place, place ^ flip) for place in range(size)])


def shift(values, axis, step):
    size = lax.axis_size(axis)
    return lax.ppermute(values, axis, [(place, (place + step) % size) for place in range(size)])


def flips(axis):
    size = lax.axis_size(axis)
    return [1 << bit for bit in range(size.bit_length() - 1)]


def gather_near(rows, axis, along=0):
    for flip in reversed(flips(axis)):
        rows = jnp.concatenate([rows, swap(rows, axis, flip)], axis=along)
    return rows


def add_near(rows, axis):
    for flip in flips(axis):
        kept = rows.shape[0] // 2
        arrived = swap(rows[kept:], axis, flip)
        rows = (rows[:kept].astype(jnp.float32) + arrived.astype(jnp.float32)).astype(jnp.bfloat16)
    return rows


def near_order(axis):
    order = [0]
    for flip in reversed(flips(axis)):
        order = order + [place ^ flip for place in order]
    return order


def attend_pieces(queries, key_pieces, value_pieces):
    head_size = queries.shape[-1]
    kv_local = queries.shape[1]
    scores = [
        jnp.einsum(
            "qgrd,kgd->grqk",
            queries,
            piece.reshape(piece.shape[0], kv_local, head_size),
            preferred_element_type=jnp.float32,
        )
        * head_size ** (-0.5)
        for piece in key_pieces
    ]
    scores = jnp.concatenate(scores, axis=-1)
    values = jnp.concatenate(value_pieces, axis=0)
    peak = jnp.max(scores, axis=-1, keepdims=True)
    weights = jnp.exp(scores - peak)
    total = jnp.sum(weights, axis=-1)
    heard = jnp.einsum(
        "grqk,kgd->qgrd",
        weights.astype(jnp.bfloat16),
        values.reshape(values.shape[0], kv_local, head_size),
        preferred_element_type=jnp.float32,
    )
    heard = heard / jnp.transpose(total, (2, 0, 1))[..., None]
    return heard.reshape(heard.shape[0], -1).astype(jnp.bfloat16)


def gather_plan(
    queries_small,
    keys_small,
    values_small,
    queries_large,
    keys_large,
    values_large,
    query_gain_small,
    key_gain_small,
    query_gain_large,
    key_gain_large,
    residual_in,
    out_weight_small,
    out_weight_large,
    norm_gain,
    routes,
    route_scores,
    expert_gate,
    expert_up,
    expert_down,
):
    token_rows = queries_small.shape[0]
    local_rows = routes.shape[0]
    sp_count = lax.axis_size("sp")
    sp_index = lax.axis_index("sp")
    tp_index = lax.axis_index("tp")
    local_experts = expert_gate.shape[0]
    steps = list(range(sp_count))
    offset = sp_index * token_rows
    tables_small = grid_tables(offset, token_rows, HS_SMALL)
    tables_large = grid_tables(offset, token_rows, HS_LARGE)
    kv_small = keys_small.shape[1] // HS_SMALL
    kv_large = keys_large.shape[1] // HS_LARGE
    turned_small = normed_turn(
        keys_small.reshape(token_rows, kv_small, HS_SMALL), key_gain_small, tables_small
    ).reshape(token_rows, -1)
    turned_large = normed_turn(
        keys_large.reshape(token_rows, kv_large, HS_LARGE), key_gain_large, tables_large
    ).reshape(token_rows, -1)
    memory = jnp.concatenate([turned_small, values_small, turned_large, values_large], axis=1)
    memories = [memory] + [shift(memory, "sp", step) for step in steps[1:]]
    cuts = [keys_small.shape[1], values_small.shape[1], keys_large.shape[1]]
    ends = [sum(cuts[: place + 1]) for place in range(3)]
    pieces = [jnp.split(rows, ends, axis=1) for rows in memories]

    shares = route_scores / jnp.sum(route_scores, axis=1, keepdims=True)
    experts = jnp.arange(local_experts * sp_count, dtype=jnp.int32)
    named = (routes[:, :, None] == experts).astype(jnp.float32)
    mixing = jnp.sum(named * shares[:, :, None], axis=1).T
    mixing = gather_near(mixing, "tp", along=1)
    mixings = [mixing] + [shift(mixing, "sp", step) for step in steps[1:]]
    mixings = [
        lax.dynamic_slice_in_dim(block, sp_index * local_experts, local_experts, 0)
        for block in mixings
    ]

    order = near_order("tp")

    def reorder(rows):
        return jnp.concatenate(
            [
                lax.dynamic_slice_in_dim(rows, (tp_index ^ place) * local_rows, local_rows, 0)
                for place in order
            ],
            axis=0,
        )

    asked_small = reorder(
        normed_turn(
            queries_small.reshape(token_rows, -1, HS_SMALL), query_gain_small, tables_small
        ).reshape(token_rows, -1)
    ).reshape(token_rows, kv_small, -1, HS_SMALL)
    asked_large = reorder(
        normed_turn(
            queries_large.reshape(token_rows, -1, HS_LARGE), query_gain_large, tables_large
        ).reshape(token_rows, -1)
    ).reshape(token_rows, kv_large, -1, HS_LARGE)
    heard_small = attend_pieces(asked_small, [p[0] for p in pieces], [p[1] for p in pieces])
    heard_large = attend_pieces(asked_large, [p[2] for p in pieces], [p[3] for p in pieces])
    terms = (
        jnp.dot(heard_small, out_weight_small, preferred_element_type=jnp.float32)
        + jnp.dot(heard_large, out_weight_large, preferred_element_type=jnp.float32)
    ).astype(jnp.bfloat16)
    for flip in flips("tp"):
        kept = terms.shape[0] // 2
        arrived = swap(terms[kept:], "tp", flip)
        terms = terms[:kept].astype(jnp.float32) + arrived.astype(jnp.float32)
        if kept > local_rows:
            terms = terms.astype(jnp.bfloat16)
    attended = (residual_in.astype(jnp.float32) + terms).astype(jnp.bfloat16)
    widened = attended.astype(jnp.float32)
    normed = (
        widened
        * lax.rsqrt(jnp.mean(widened * widened, axis=-1, keepdims=True) + norm_eps)
        * norm_gain
    ).astype(jnp.bfloat16)

    arrivals = [normed] + [shift(normed, "sp", step) for step in steps[1:]]
    total = attended.astype(jnp.float32)
    for step in steps:
        rows = gather_near(arrivals[step], "tp")
        actives = []
        for place in range(local_experts):
            gate_out = jnp.dot(rows, expert_gate[place], preferred_element_type=jnp.float32)
            up_out = jnp.dot(rows, expert_up[place], preferred_element_type=jnp.float32)
            actives.append(
                (jax.nn.silu(gate_out) * up_out * mixings[step][place][:, None]).astype(
                    jnp.bfloat16
                )
            )
        down = expert_down.reshape(-1, expert_down.shape[2])
        partial = jnp.dot(
            jnp.concatenate(actives, axis=1), down, preferred_element_type=jnp.float32
        ).astype(jnp.bfloat16)
        summed = add_near(partial, "tp")
        if step:
            summed = shift(summed, "sp", -step)
        total = total + summed.astype(jnp.float32)
    return total.astype(jnp.bfloat16)


def on_device(*arrays):
    routes, expert_gate = arrays[14], arrays[16]
    devices = lax.axis_size("sp") * lax.axis_size("tp")
    tokens = routes.shape[0] * devices
    expert_count = expert_gate.shape[0] * lax.axis_size("sp")
    capacity = max(2, (2 * routes.size + expert_count - 1) // expert_count)
    slots = devices * expert_gate.shape[0] * capacity
    tp_size = lax.axis_size("tp")
    if tokens <= slots and tp_size & (tp_size - 1) == 0:
        return gather_plan(*arrays)
    return dispatch_plan(*arrays)


def solution(mesh):
    in_specs = (
        P(("grp", "sp"), "tp"),
        P(("grp", "sp"), "tp"),
        P(("grp", "sp"), "tp"),
        P(("grp", "sp"), "tp"),
        P(("grp", "sp"), "tp"),
        P(("grp", "sp"), "tp"),
        P("grp"),
        P("grp"),
        P("grp"),
        P("grp"),
        P(("grp", "sp", "tp"), None),
        P("tp", None),
        P("tp", None),
        P(),
        P(("grp", "sp", "tp"), None),
        P(("grp", "sp", "tp"), None),
        P("sp", None, "tp"),
        P("sp", None, "tp"),
        P("sp", "tp", None),
    )
    out_specs = P(("grp", "sp", "tp"), None)
    return jax.shard_map(
        on_device, mesh=mesh, in_specs=in_specs, out_specs=out_specs, check_vma=False
    )
```

```python
import jax
import jax.numpy as jnp
from jax import lax
from jax.sharding import PartitionSpec as P


HS_SMALL = 64
HS_LARGE = 128
GRID_W = 64


theta_base = 10000.0
norm_eps = 1e-06
block_target = 1280


def grid_tables(offset, length, head_size):
    places = offset + jnp.arange(length, dtype=jnp.int32)
    grid_rows = (places // GRID_W).astype(jnp.float32)
    grid_cols = (places % GRID_W).astype(jnp.float32)
    rates = jnp.power(
        theta_base, -2.0 * jnp.arange(head_size // 4, dtype=jnp.float32) / (head_size // 2)
    )
    row_angles = grid_rows[:, None, None] * rates
    col_angles = grid_cols[:, None, None] * rates
    return (jnp.cos(row_angles), jnp.sin(row_angles), jnp.cos(col_angles), jnp.sin(col_angles))


def half_turn(segment, cosine, sine_part):
    half_size = segment.shape[-1] // 2
    leading = segment[..., :half_size]
    trailing = segment[..., half_size:]
    return jnp.concatenate(
        [leading * cosine - trailing * sine_part, trailing * cosine + leading * sine_part], axis=-1
    )


def grid_turn(vectors, tables):
    row_cos, row_sin, col_cos, col_sin = tables
    half_size = vectors.shape[-1] // 2
    return jnp.concatenate(
        [
            half_turn(vectors[..., :half_size], row_cos, row_sin),
            half_turn(vectors[..., half_size:], col_cos, col_sin),
        ],
        axis=-1,
    )


def normed_turn(raw_rows, gain, tables):
    widened = raw_rows.astype(jnp.float32)
    scaled = (
        widened * lax.rsqrt(jnp.mean(widened * widened, axis=-1, keepdims=True) + norm_eps) * gain
    )
    return grid_turn(scaled, tables).astype(jnp.bfloat16)


def block_rows(row_count, shard_rows):
    shards = row_count // shard_rows
    chosen = 1
    for factor in range(1, max(1, block_target // shard_rows) + 1):
        if shards % factor == 0:
            chosen = factor
    return chosen * shard_rows


def attend_block(state, queries, key_rows, value_rows):
    largest, weight_sum, accumulated = state
    head_size = queries.shape[-1]
    kv_local = queries.shape[1]
    key_heads = key_rows.reshape(key_rows.shape[0], kv_local, head_size)
    value_heads = value_rows.reshape(value_rows.shape[0], kv_local, head_size)
    scores = jnp.einsum(
        "qgrd,kgd->qgrk", queries, key_heads, preferred_element_type=jnp.float32
    ) * head_size ** (-0.5)
    peak_score = jnp.maximum(largest, jnp.max(scores, axis=-1))
    shrink = jnp.exp(largest - peak_score)
    weights = jnp.exp(scores - peak_score[..., None])
    weight_sum = weight_sum * shrink + jnp.sum(weights, axis=-1)
    accumulated = accumulated * shrink[..., None] + jnp.einsum(
        "qgrk,kgd->qgrd",
        weights.astype(jnp.bfloat16),
        value_heads,
        preferred_element_type=jnp.float32,
    )
    return (peak_score, weight_sum, accumulated)


def attend_rows(state, queries, key_rows, value_rows):
    row_count = key_rows.shape[0]
    step_rows = block_rows(row_count, queries.shape[0])
    if step_rows == row_count:
        return attend_block(state, queries, key_rows, value_rows)

    def one_block(block_index, carried):
        offset = block_index * step_rows
        return attend_block(
            carried,
            queries,
            lax.dynamic_slice_in_dim(key_rows, offset, step_rows, 0),
            lax.dynamic_slice_in_dim(value_rows, offset, step_rows, 0),
        )

    return lax.fori_loop(0, row_count // step_rows, one_block, state)


def empty_state(queries):
    state_shape = queries.shape[:3]
    return (
        jnp.full(state_shape, -1e30, jnp.float32),
        jnp.zeros(state_shape, jnp.float32),
        jnp.zeros(queries.shape, jnp.float32),
    )


def finish(state):
    _, weight_sum, accumulated = state
    merged = accumulated / weight_sum[..., None]
    return merged.reshape(merged.shape[0], -1).astype(jnp.bfloat16)


def dispatch_plan(
    queries_small,
    keys_small,
    values_small,
    queries_large,
    keys_large,
    values_large,
    query_gain_small,
    key_gain_small,
    query_gain_large,
    key_gain_large,
    residual_in,
    out_weight_small,
    out_weight_large,
    norm_gain,
    routes,
    route_scores,
    expert_gate,
    expert_up,
    expert_down,
):
    token_rows = queries_small.shape[0]
    offset = lax.axis_index("sp") * token_rows
    tables_small = grid_tables(offset, token_rows, HS_SMALL)
    tables_large = grid_tables(offset, token_rows, HS_LARGE)
    kv_small = keys_small.shape[1] // HS_SMALL
    kv_large = keys_large.shape[1] // HS_LARGE
    asked_small = normed_turn(
        queries_small.reshape(token_rows, -1, HS_SMALL), query_gain_small, tables_small
    ).reshape(token_rows, kv_small, -1, HS_SMALL)
    asked_large = normed_turn(
        queries_large.reshape(token_rows, -1, HS_LARGE), query_gain_large, tables_large
    ).reshape(token_rows, kv_large, -1, HS_LARGE)
    turned_small = normed_turn(
        keys_small.reshape(token_rows, kv_small, HS_SMALL), key_gain_small, tables_small
    ).reshape(token_rows, -1)
    turned_large = normed_turn(
        keys_large.reshape(token_rows, kv_large, HS_LARGE), key_gain_large, tables_large
    ).reshape(token_rows, -1)
    key_small = lax.all_gather(turned_small, "sp", axis=0, tiled=True)
    value_small = lax.all_gather(values_small, "sp", axis=0, tiled=True)
    key_large = lax.all_gather(turned_large, "sp", axis=0, tiled=True)
    value_large = lax.all_gather(values_large, "sp", axis=0, tiled=True)
    state_small = attend_rows(empty_state(asked_small), asked_small, key_small, value_small)
    state_large = attend_rows(empty_state(asked_large), asked_large, key_large, value_large)
    heard_small = finish(state_small)
    heard_large = finish(state_large)
    projected = lax.psum_scatter(
        (
            jnp.dot(heard_small, out_weight_small, preferred_element_type=jnp.float32)
            + jnp.dot(heard_large, out_weight_large, preferred_element_type=jnp.float32)
        ).astype(jnp.bfloat16),
        "tp",
        scatter_dimension=0,
        tiled=True,
    ).astype(jnp.float32)
    attended = (residual_in.astype(jnp.float32) + projected).astype(jnp.bfloat16)
    widened = attended.astype(jnp.float32)
    normed = (
        widened
        * lax.rsqrt(jnp.mean(widened * widened, axis=-1, keepdims=True) + norm_eps)
        * norm_gain
    ).astype(jnp.bfloat16)
    local_rows = routes.shape[0]
    top_count = routes.shape[1]
    sp_count = lax.axis_size("sp")
    local_experts = expert_gate.shape[0]
    expert_count = local_experts * sp_count
    capacity = max(2, (2 * top_count * local_rows + expert_count - 1) // expert_count)
    flat_routes = routes.reshape(-1)
    member = (flat_routes[:, None] == jnp.arange(expert_count, dtype=jnp.int32)[None, :]).astype(
        jnp.int32
    )
    ranks = jnp.sum((jnp.cumsum(member, axis=0) - member) * member, axis=1)
    slots = flat_routes * capacity + ranks
    picker = (
        slots[:, None] == jnp.arange(expert_count * capacity, dtype=jnp.int32)[None, :]
    ).astype(jnp.bfloat16)
    placer = jnp.sum(picker.reshape(local_rows, top_count, -1), axis=1)
    outgoing = jnp.einsum("ts,td->sd", placer, normed, preferred_element_type=jnp.float32).astype(
        jnp.bfloat16
    )
    outgoing = outgoing.reshape(sp_count, local_experts, capacity, -1)
    everyone = lax.all_gather(
        lax.all_to_all(outgoing, "sp", split_axis=0, concat_axis=0, tiled=True),
        "tp",
        axis=0,
        tiled=True,
    )
    gate_out = jnp.einsum(
        "secd,edf->secf", everyone, expert_gate, preferred_element_type=jnp.float32
    )
    up_out = jnp.einsum("secd,edf->secf", everyone, expert_up, preferred_element_type=jnp.float32)
    active = (jax.nn.silu(gate_out) * up_out).astype(jnp.bfloat16)
    summed = lax.psum_scatter(
        jnp.einsum(
            "secf,efd->secd", active, expert_down, preferred_element_type=jnp.float32
        ).astype(jnp.bfloat16),
        "tp",
        scatter_dimension=0,
        tiled=True,
    )
    returned = lax.all_to_all(summed, "sp", split_axis=0, concat_axis=0, tiled=True)
    back_rows = returned.reshape(expert_count * capacity, -1)
    chosen_rows = jnp.dot(picker, back_rows, preferred_element_type=jnp.float32).reshape(
        local_rows, top_count, -1
    )
    shares = route_scores / jnp.sum(route_scores, axis=1, keepdims=True)
    mixed = jnp.sum(chosen_rows * shares[:, :, None], axis=1)
    return (attended.astype(jnp.float32) + mixed).astype(jnp.bfloat16)


def swap(values, axis, flip):
    size = lax.axis_size(axis)
    return lax.ppermute(values, axis, [(place, place ^ flip) for place in range(size)])


def shift(values, axis, step):
    size = lax.axis_size(axis)
    pairs = [(place, (place + step) % size) for place in range(size)]
    return lax.ppermute(values, axis, pairs)


def flips(axis):
    size = lax.axis_size(axis)
    return [1 << bit for bit in range(size.bit_length() - 1)]


def gather_near(rows, axis, along=0):
    for flip in reversed(flips(axis)):
        arrived = swap(rows, axis, flip)
        rows = jnp.concatenate([rows, arrived], axis=along)
    return rows


def add_near(make, row_count):
    axis = "tp"
    half = row_count // 2
    kept, given = None, None
    for flip in flips(axis):
        if kept is None:
            given = make(half, row_count)
            arrived = swap(given, axis, flip)
            kept = make(0, half).astype(jnp.float32) + arrived.astype(jnp.float32)
        else:
            half = kept.shape[0] // 2
            kept = kept.astype(jnp.bfloat16)
            arrived = swap(kept[half:], axis, flip)
            kept = kept[:half].astype(jnp.float32) + arrived.astype(jnp.float32)
    return kept


def near_order(axis):
    order = [0]
    for flip in reversed(flips(axis)):
        order = order + [place ^ flip for place in order]
    return order


def attend_pieces(queries, key_pieces, value_pieces):
    head_size = queries.shape[-1]
    kv_local = queries.shape[1]
    scores = [
        jnp.einsum(
            "qgrd,kgd->grqk",
            queries,
            piece.reshape(piece.shape[0], kv_local, head_size),
            preferred_element_type=jnp.float32,
        )
        * head_size ** (-0.5)
        for piece in key_pieces
    ]
    scores = jnp.concatenate(scores, axis=-1)
    values = jnp.concatenate(value_pieces, axis=0)
    peak = jnp.max(scores, axis=-1, keepdims=True)
    weights = jnp.exp(scores - peak)
    total = jnp.sum(weights, axis=-1)
    heard = jnp.einsum(
        "grqk,kgd->qgrd",
        weights.astype(jnp.bfloat16),
        values.reshape(values.shape[0], kv_local, head_size),
        preferred_element_type=jnp.float32,
    )
    heard = heard / jnp.transpose(total, (2, 0, 1))[..., None]
    return heard.reshape(heard.shape[0], -1).astype(jnp.bfloat16)


def gather_plan(
    queries_small,
    keys_small,
    values_small,
    queries_large,
    keys_large,
    values_large,
    query_gain_small,
    key_gain_small,
    query_gain_large,
    key_gain_large,
    residual_in,
    out_weight_small,
    out_weight_large,
    norm_gain,
    routes,
    route_scores,
    expert_gate,
    expert_up,
    expert_down,
):
    token_rows = queries_small.shape[0]
    local_rows = routes.shape[0]
    sp_count = lax.axis_size("sp")
    sp_index = lax.axis_index("sp")
    tp_index = lax.axis_index("tp")
    local_experts = expert_gate.shape[0]
    steps = list(range(sp_count))
    offset = sp_index * token_rows
    tables_small = grid_tables(offset, token_rows, HS_SMALL)
    tables_large = grid_tables(offset, token_rows, HS_LARGE)
    kv_small = keys_small.shape[1] // HS_SMALL
    kv_large = keys_large.shape[1] // HS_LARGE
    turned_small = normed_turn(
        keys_small.reshape(token_rows, kv_small, HS_SMALL), key_gain_small, tables_small
    ).reshape(token_rows, -1)
    turned_large = normed_turn(
        keys_large.reshape(token_rows, kv_large, HS_LARGE), key_gain_large, tables_large
    ).reshape(token_rows, -1)
    memory = jnp.concatenate([turned_small, values_small, turned_large, values_large], axis=1)
    memories = [memory] + [shift(memory, "sp", step) for step in steps[1:]]
    cuts = [keys_small.shape[1], values_small.shape[1], keys_large.shape[1]]
    ends = [sum(cuts[: place + 1]) for place in range(3)]
    pieces = [jnp.split(rows, ends, axis=1) for rows in memories]

    shares = route_scores / jnp.sum(route_scores, axis=1, keepdims=True)
    experts = jnp.arange(local_experts * sp_count, dtype=jnp.int32)
    named = (routes[:, :, None] == experts).astype(jnp.float32)
    mixing = jnp.sum(named * shares[:, :, None], axis=1).T
    mixing = gather_near(mixing, "tp", along=1)
    mixings = [mixing] + [shift(mixing, "sp", step) for step in steps[1:]]
    mixings = [
        lax.dynamic_slice_in_dim(block, sp_index * local_experts, local_experts, 0)
        for block in mixings
    ]

    order = near_order("tp")

    def reorder(rows):
        return jnp.concatenate(
            [
                lax.dynamic_slice_in_dim(rows, (tp_index ^ place) * local_rows, local_rows, 0)
                for place in order
            ],
            axis=0,
        )

    asked_small = reorder(
        normed_turn(
            queries_small.reshape(token_rows, -1, HS_SMALL), query_gain_small, tables_small
        ).reshape(token_rows, -1)
    ).reshape(token_rows, kv_small, -1, HS_SMALL)
    asked_large = reorder(
        normed_turn(
            queries_large.reshape(token_rows, -1, HS_LARGE), query_gain_large, tables_large
        ).reshape(token_rows, -1)
    ).reshape(token_rows, kv_large, -1, HS_LARGE)
    heard_small = attend_pieces(asked_small, [p[0] for p in pieces], [p[1] for p in pieces])
    heard_large = attend_pieces(asked_large, [p[2] for p in pieces], [p[3] for p in pieces])

    def project(first, last):
        return (
            jnp.dot(
                heard_small[first:last], out_weight_small, preferred_element_type=jnp.float32
            )
            + jnp.dot(
                heard_large[first:last], out_weight_large, preferred_element_type=jnp.float32
            )
        ).astype(jnp.bfloat16)

    attended = add_near(project, token_rows)
    attended = (residual_in.astype(jnp.float32) + attended).astype(jnp.bfloat16)
    widened = attended.astype(jnp.float32)
    normed = (
        widened
        * lax.rsqrt(jnp.mean(widened * widened, axis=-1, keepdims=True) + norm_eps)
        * norm_gain
    ).astype(jnp.bfloat16)

    arrivals = [normed] + [shift(normed, "sp", step) for step in steps[1:]]
    down = expert_down.reshape(-1, expert_down.shape[2])
    total = attended.astype(jnp.float32)
    for step in steps:
        rows = lax.optimization_barrier(gather_near(arrivals[step], "tp"))
        actives = []
        for place in range(local_experts):
            gate_out = jnp.dot(rows, expert_gate[place], preferred_element_type=jnp.float32)
            up_out = jnp.dot(rows, expert_up[place], preferred_element_type=jnp.float32)
            actives.append(
                (jax.nn.silu(gate_out) * up_out * mixings[step][place][:, None]).astype(
                    jnp.bfloat16
                )
            )
        actives = jnp.concatenate(actives, axis=1)

        def finish_rows(first, last):
            return jnp.dot(
                actives[first:last], down, preferred_element_type=jnp.float32
            ).astype(jnp.bfloat16)

        summed = add_near(finish_rows, token_rows)
        if step:
            summed = shift(summed.astype(jnp.bfloat16), "sp", -step)
        total = total + summed.astype(jnp.float32)
    return total.astype(jnp.bfloat16)


def on_device(*arrays):
    routes, expert_gate = arrays[14], arrays[16]
    devices = lax.axis_size("sp") * lax.axis_size("tp")
    tokens = routes.shape[0] * devices
    expert_count = expert_gate.shape[0] * lax.axis_size("sp")
    capacity = max(2, (2 * routes.size + expert_count - 1) // expert_count)
    slots = devices * expert_gate.shape[0] * capacity
    tp_size = lax.axis_size("tp")
    if tokens <= slots and tp_size & (tp_size - 1) == 0:
        return gather_plan(*arrays)
    return dispatch_plan(*arrays)


def solution(mesh):
    in_specs = (
        P(("grp", "sp"), "tp"),
        P(("grp", "sp"), "tp"),
        P(("grp", "sp"), "tp"),
        P(("grp", "sp"), "tp"),
        P(("grp", "sp"), "tp"),
        P(("grp", "sp"), "tp"),
        P("grp"),
        P("grp"),
        P("grp"),
        P("grp"),
        P(("grp", "sp", "tp"), None),
        P("tp", None),
        P("tp", None),
        P(),
        P(("grp", "sp", "tp"), None),
        P(("grp", "sp", "tp"), None),
        P("sp", None, "tp"),
        P("sp", None, "tp"),
        P("sp", "tp", None),
    )
    out_specs = P(("grp", "sp", "tp"), None)
    return jax.shard_map(
        on_device, mesh=mesh, in_specs=in_specs, out_specs=out_specs, check_vma=False
    )
```

```python
import jax
import jax.numpy as jnp
import numpy as np
from jax import lax
from jax.experimental import pallas as pl
from jax.experimental.pallas import tpu as pltpu
from jax.sharding import PartitionSpec as P


HS_SMALL = 64
HS_LARGE = 128
GRID_W = 64


theta_base = 10000.0
norm_eps = 1e-06
block_target = 1280


def grid_tables(offset, length, head_size):
    places = offset + jnp.arange(length, dtype=jnp.int32)
    grid_rows = (places // GRID_W).astype(jnp.float32)
    grid_cols = (places % GRID_W).astype(jnp.float32)
    rates = jnp.power(
        theta_base, -2.0 * jnp.arange(head_size // 4, dtype=jnp.float32) / (head_size // 2)
    )
    row_angles = grid_rows[:, None, None] * rates
    col_angles = grid_cols[:, None, None] * rates
    return (jnp.cos(row_angles), jnp.sin(row_angles), jnp.cos(col_angles), jnp.sin(col_angles))


def half_turn(segment, cosine, sine_part):
    half_size = segment.shape[-1] // 2
    leading = segment[..., :half_size]
    trailing = segment[..., half_size:]
    return jnp.concatenate(
        [leading * cosine - trailing * sine_part, trailing * cosine + leading * sine_part], axis=-1
    )


def grid_turn(vectors, tables):
    row_cos, row_sin, col_cos, col_sin = tables
    half_size = vectors.shape[-1] // 2
    return jnp.concatenate(
        [
            half_turn(vectors[..., :half_size], row_cos, row_sin),
            half_turn(vectors[..., half_size:], col_cos, col_sin),
        ],
        axis=-1,
    )


def normed_turn(raw_rows, gain, tables):
    widened = raw_rows.astype(jnp.float32)
    scaled = (
        widened * lax.rsqrt(jnp.mean(widened * widened, axis=-1, keepdims=True) + norm_eps) * gain
    )
    return grid_turn(scaled, tables).astype(jnp.bfloat16)


def block_rows(row_count, shard_rows):
    shards = row_count // shard_rows
    chosen = 1
    for factor in range(1, max(1, block_target // shard_rows) + 1):
        if shards % factor == 0:
            chosen = factor
    return chosen * shard_rows


def attend_block(state, queries, key_rows, value_rows):
    largest, weight_sum, accumulated = state
    head_size = queries.shape[-1]
    kv_local = queries.shape[1]
    key_heads = key_rows.reshape(key_rows.shape[0], kv_local, head_size)
    value_heads = value_rows.reshape(value_rows.shape[0], kv_local, head_size)
    scores = jnp.einsum(
        "qgrd,kgd->qgrk", queries, key_heads, preferred_element_type=jnp.float32
    ) * head_size ** (-0.5)
    peak_score = jnp.maximum(largest, jnp.max(scores, axis=-1))
    shrink = jnp.exp(largest - peak_score)
    weights = jnp.exp(scores - peak_score[..., None])
    weight_sum = weight_sum * shrink + jnp.sum(weights, axis=-1)
    accumulated = accumulated * shrink[..., None] + jnp.einsum(
        "qgrk,kgd->qgrd",
        weights.astype(jnp.bfloat16),
        value_heads,
        preferred_element_type=jnp.float32,
    )
    return (peak_score, weight_sum, accumulated)


def attend_rows(state, queries, key_rows, value_rows):
    row_count = key_rows.shape[0]
    step_rows = block_rows(row_count, queries.shape[0])
    if step_rows == row_count:
        return attend_block(state, queries, key_rows, value_rows)

    def one_block(block_index, carried):
        offset = block_index * step_rows
        return attend_block(
            carried,
            queries,
            lax.dynamic_slice_in_dim(key_rows, offset, step_rows, 0),
            lax.dynamic_slice_in_dim(value_rows, offset, step_rows, 0),
        )

    return lax.fori_loop(0, row_count // step_rows, one_block, state)


def empty_state(queries):
    state_shape = queries.shape[:3]
    return (
        jnp.full(state_shape, -1e30, jnp.float32),
        jnp.zeros(state_shape, jnp.float32),
        jnp.zeros(queries.shape, jnp.float32),
    )


def finish(state):
    _, weight_sum, accumulated = state
    merged = accumulated / weight_sum[..., None]
    return merged.reshape(merged.shape[0], -1).astype(jnp.bfloat16)


def dispatch_plan(
    queries_small,
    keys_small,
    values_small,
    queries_large,
    keys_large,
    values_large,
    query_gain_small,
    key_gain_small,
    query_gain_large,
    key_gain_large,
    residual_in,
    out_weight_small,
    out_weight_large,
    norm_gain,
    routes,
    route_scores,
    expert_gate,
    expert_up,
    expert_down,
):
    token_rows = queries_small.shape[0]
    offset = lax.axis_index("sp") * token_rows
    tables_small = grid_tables(offset, token_rows, HS_SMALL)
    tables_large = grid_tables(offset, token_rows, HS_LARGE)
    kv_small = keys_small.shape[1] // HS_SMALL
    kv_large = keys_large.shape[1] // HS_LARGE
    asked_small = normed_turn(
        queries_small.reshape(token_rows, -1, HS_SMALL), query_gain_small, tables_small
    ).reshape(token_rows, kv_small, -1, HS_SMALL)
    asked_large = normed_turn(
        queries_large.reshape(token_rows, -1, HS_LARGE), query_gain_large, tables_large
    ).reshape(token_rows, kv_large, -1, HS_LARGE)
    turned_small = normed_turn(
        keys_small.reshape(token_rows, kv_small, HS_SMALL), key_gain_small, tables_small
    ).reshape(token_rows, -1)
    turned_large = normed_turn(
        keys_large.reshape(token_rows, kv_large, HS_LARGE), key_gain_large, tables_large
    ).reshape(token_rows, -1)
    key_small = lax.all_gather(turned_small, "sp", axis=0, tiled=True)
    value_small = lax.all_gather(values_small, "sp", axis=0, tiled=True)
    key_large = lax.all_gather(turned_large, "sp", axis=0, tiled=True)
    value_large = lax.all_gather(values_large, "sp", axis=0, tiled=True)
    state_small = attend_rows(empty_state(asked_small), asked_small, key_small, value_small)
    state_large = attend_rows(empty_state(asked_large), asked_large, key_large, value_large)
    heard_small = finish(state_small)
    heard_large = finish(state_large)
    projected = lax.psum_scatter(
        (
            jnp.dot(heard_small, out_weight_small, preferred_element_type=jnp.float32)
            + jnp.dot(heard_large, out_weight_large, preferred_element_type=jnp.float32)
        ).astype(jnp.bfloat16),
        "tp",
        scatter_dimension=0,
        tiled=True,
    ).astype(jnp.float32)
    attended = (residual_in.astype(jnp.float32) + projected).astype(jnp.bfloat16)
    widened = attended.astype(jnp.float32)
    normed = (
        widened
        * lax.rsqrt(jnp.mean(widened * widened, axis=-1, keepdims=True) + norm_eps)
        * norm_gain
    ).astype(jnp.bfloat16)
    local_rows = routes.shape[0]
    top_count = routes.shape[1]
    sp_count = lax.axis_size("sp")
    local_experts = expert_gate.shape[0]
    expert_count = local_experts * sp_count
    capacity = max(2, (2 * top_count * local_rows + expert_count - 1) // expert_count)
    flat_routes = routes.reshape(-1)
    member = (flat_routes[:, None] == jnp.arange(expert_count, dtype=jnp.int32)[None, :]).astype(
        jnp.int32
    )
    ranks = jnp.sum((jnp.cumsum(member, axis=0) - member) * member, axis=1)
    slots = flat_routes * capacity + ranks
    picker = (
        slots[:, None] == jnp.arange(expert_count * capacity, dtype=jnp.int32)[None, :]
    ).astype(jnp.bfloat16)
    placer = jnp.sum(picker.reshape(local_rows, top_count, -1), axis=1)
    outgoing = jnp.einsum("ts,td->sd", placer, normed, preferred_element_type=jnp.float32).astype(
        jnp.bfloat16
    )
    outgoing = outgoing.reshape(sp_count, local_experts, capacity, -1)
    everyone = lax.all_gather(
        lax.all_to_all(outgoing, "sp", split_axis=0, concat_axis=0, tiled=True),
        "tp",
        axis=0,
        tiled=True,
    )
    gate_out = jnp.einsum(
        "secd,edf->secf", everyone, expert_gate, preferred_element_type=jnp.float32
    )
    up_out = jnp.einsum("secd,edf->secf", everyone, expert_up, preferred_element_type=jnp.float32)
    active = (jax.nn.silu(gate_out) * up_out).astype(jnp.bfloat16)
    summed = lax.psum_scatter(
        jnp.einsum(
            "secf,efd->secd", active, expert_down, preferred_element_type=jnp.float32
        ).astype(jnp.bfloat16),
        "tp",
        scatter_dimension=0,
        tiled=True,
    )
    returned = lax.all_to_all(summed, "sp", split_axis=0, concat_axis=0, tiled=True)
    back_rows = returned.reshape(expert_count * capacity, -1)
    chosen_rows = jnp.dot(picker, back_rows, preferred_element_type=jnp.float32).reshape(
        local_rows, top_count, -1
    )
    shares = route_scores / jnp.sum(route_scores, axis=1, keepdims=True)
    mixed = jnp.sum(chosen_rows * shares[:, :, None], axis=1)
    return (attended.astype(jnp.float32) + mixed).astype(jnp.bfloat16)


def swap(values, axis, flip):
    size = lax.axis_size(axis)
    return lax.ppermute(values, axis, [(place, place ^ flip) for place in range(size)])


def meet(values, flip):
    return swap(values, "sp", flip)


def inner_meet(values):
    return lax.ppermute(values, "sp", [(0, 0), (1, 2), (2, 1), (3, 3)])


def is_inner():
    place = lax.axis_index("sp")
    return jnp.logical_or(place == 1, place == 2)


def flips(axis):
    size = lax.axis_size(axis)
    return [1 << bit for bit in range(size.bit_length() - 1)]


def gather_near(rows, axis, along=0):
    for flip in reversed(flips(axis)):
        arrived = swap(rows, axis, flip)
        rows = jnp.concatenate([rows, arrived], axis=along)
    return rows


def add_near(make, row_count):
    axis = "tp"
    half = row_count // 2
    kept, given = None, None
    for flip in flips(axis):
        if kept is None:
            given = make(half, row_count)
            arrived = swap(given, axis, flip)
            kept = make(0, half).astype(jnp.float32) + arrived.astype(jnp.float32)
        else:
            half = kept.shape[0] // 2
            kept = kept.astype(jnp.bfloat16)
            arrived = swap(kept[half:], axis, flip)
            kept = kept[:half].astype(jnp.float32) + arrived.astype(jnp.float32)
    return kept


def near_order(axis):
    order = [0]
    for flip in reversed(flips(axis)):
        order = order + [place ^ flip for place in order]
    return order


LANES = 128


def turn_tables(head_size, rows):
    quarter = head_size // 4
    lane = np.arange(LANES) % head_size
    rate = theta_base ** (-2.0 * (lane % quarter) / (head_size // 2))
    sign = np.where((lane // quarter) % 2 == 0, -1.0, 1.0)

    def pair(count):
        angles = np.arange(count)[:, None] * rate
        return [np.cos(angles).astype(np.float32), (np.sin(angles) * sign).astype(np.float32)]

    return pair(rows) + pair(GRID_W)


def swap_quarters(rows, head_size):
    quarter = head_size // 4
    lane = lax.broadcasted_iota(jnp.int32, rows.shape, 1)
    ahead = pltpu.roll(rows, LANES - quarter, 1)
    behind = pltpu.roll(rows, quarter, 1)
    return jnp.where((lane // quarter) % 2 == 0, ahead, behind)


def turn_block(raw, gain, head_size, cosine, sine):
    rows = raw.astype(jnp.float32)
    squares = rows * rows
    lane = lax.broadcasted_iota(jnp.int32, rows.shape, 1)
    means = None
    for head in range(LANES // head_size):
        inside = (lane // head_size) == head
        mean = jnp.sum(jnp.where(inside, squares, 0.0), axis=1, keepdims=True) / head_size
        means = mean if means is None else jnp.where(inside, mean, means)
    scaled = rows * lax.rsqrt(means + norm_eps) * gain
    return (scaled * cosine + swap_quarters(scaled, head_size) * sine).astype(jnp.bfloat16)


def lane_tables(first_row, blocks, head_size, refs):
    row_cos, row_sin, col_cos, col_sin = refs
    lane = lax.broadcasted_iota(jnp.int32, (GRID_W, LANES), 1)
    by_row = (lane % head_size) < head_size // 2
    cosines, sines = [], []
    for block in range(blocks):
        row = pl.ds(first_row + block, 1)
        cosines.append(jnp.where(by_row, row_cos[row, :], col_cos[...]))
        sines.append(jnp.where(by_row, row_sin[row, :], col_sin[...]))
    return jnp.concatenate(cosines, axis=0), jnp.concatenate(sines, axis=0)


def key_kernel(*refs):
    sources, (memory,), held, sems = refs[:7], refs[7:8], refs[8:13], refs[13]
    keys_s, keys_l, gain_s, gain_l, tables = held
    targets = [
        keys_s,
        memory.at[:, LANES : 2 * LANES],
        keys_l,
        memory.at[:, 3 * LANES :],
        gain_s,
        gain_l,
        tables,
    ]
    copies = [
        pltpu.make_async_copy(source, target, sems.at[place])
        for place, (source, target) in enumerate(zip(sources, targets))
    ]
    for copy in copies:
        copy.start()
    for copy in copies:
        copy.wait()
    blocks = memory.shape[0] // GRID_W
    first = lax.axis_index("sp") * blocks
    rows = tables.shape[0] // 4 - GRID_W
    place = 0
    parts = []
    for count in (rows, rows, GRID_W, GRID_W) * 2:
        parts.append(tables.at[place : place + count])
        place += count
    gain = jnp.concatenate([gain_s[...]] * (LANES // HS_SMALL), axis=1)
    cosine, sine = lane_tables(first, blocks, HS_SMALL, parts[:4])
    memory[:, :LANES] = turn_block(keys_s[...], gain, HS_SMALL, cosine, sine)
    cosine, sine = lane_tables(first, blocks, HS_LARGE, parts[4:])
    memory[:, 2 * LANES : 3 * LANES] = turn_block(
        keys_l[...], gain_l[...], HS_LARGE, cosine, sine
    )


def make_memory(keys_s, values_s, keys_l, values_l, gain_s, gain_l, rows):
    rows = (rows + 7) // 8 * 8
    tables = np.concatenate(turn_tables(HS_SMALL, rows) + turn_tables(HS_LARGE, rows))
    operands = (keys_s, values_s, keys_l, values_l, gain_s[None, :], gain_l[None, :], tables)
    held = [operands[place] for place in (0, 2, 4, 5, 6)]
    return pl.pallas_call(
        key_kernel,
        out_shape=jax.ShapeDtypeStruct((keys_s.shape[0], 4 * LANES), jnp.bfloat16),
        in_specs=[pl.BlockSpec(memory_space=pl.ANY)] * len(operands),
        out_specs=pl.BlockSpec(memory_space=pltpu.VMEM),
        scratch_shapes=[pltpu.VMEM(array.shape, array.dtype) for array in held]
        + [pltpu.SemaphoreType.DMA((len(operands),))],
        name="keys",
        cost_estimate=pl.CostEstimate(flops=4000000, bytes_accessed=1000000, transcendentals=0),
    )(*operands)


def attend_kernel(asked_s, asked_l, *rest):
    heard_s, heard_l, last = rest[5:]
    inner = is_inner()

    @pl.when(inner)
    def _():
        last[...] = rest[3][...]

    @pl.when(jnp.logical_not(inner))
    def _():
        last[...] = rest[4][...]

    memories = (rest[0], rest[1], rest[2], last)
    rows = asked_s.shape[0]
    low = lax.broadcasted_iota(jnp.int32, (rows, LANES), 1) < HS_SMALL

    def attend(queries, key_at, scale):
        factor = scale * 1.4426950408889634
        scores = [
            lax.dot_general(
                queries,
                memory[:, key_at : key_at + LANES],
                (((1,), (1,)), ((), ())),
                preferred_element_type=jnp.float32,
            )
            for memory in memories
        ]
        peak = scores[0]
        for piece in scores[1:]:
            peak = jnp.maximum(peak, piece)
        peak = jnp.max(peak, axis=1, keepdims=True)
        total, heard = None, None
        for piece, memory in zip(scores, memories):
            weights = jnp.exp2((piece - peak) * factor)
            total = weights if total is None else total + weights
            part = jnp.dot(
                weights.astype(jnp.bfloat16),
                memory[:, key_at + LANES : key_at + 2 * LANES],
                preferred_element_type=jnp.float32,
            )
            heard = part if heard is None else heard + part
        return heard / jnp.sum(total, axis=1, keepdims=True)

    zero = jnp.zeros((rows, LANES), jnp.float32)
    for side in range(2):
        both = asked_s[:, side * LANES : (side + 1) * LANES].astype(jnp.float32)
        turned = pltpu.roll(both, HS_SMALL, 1)
        here = low if side == 0 else jnp.logical_not(low)
        first, second = (both, turned) if side == 0 else (turned, both)
        first = jnp.where(here, first, zero).astype(jnp.bfloat16)
        second = jnp.where(here, second, zero).astype(jnp.bfloat16)
        one = attend(first, 0, HS_SMALL**-0.5)
        two = attend(second, 0, HS_SMALL**-0.5)
        if side == 0:
            two = pltpu.roll(two, HS_SMALL, 1)
        else:
            one = pltpu.roll(one, HS_SMALL, 1)
        heard_s[:, side * LANES : (side + 1) * LANES] = jnp.where(low, one, two).astype(
            jnp.bfloat16
        )
    for head in range(asked_l.shape[1] // LANES):
        lanes = slice(head * LANES, (head + 1) * LANES)
        heard_l[:, lanes] = attend(asked_l[:, lanes], 2 * LANES, HS_LARGE**-0.5).astype(
            jnp.bfloat16
        )


def attend_all(asked_s, asked_l, memories):
    rows = asked_s.shape[0]
    vmem = pl.BlockSpec(memory_space=pltpu.VMEM)
    shapes = [jax.ShapeDtypeStruct(a.shape, jnp.bfloat16) for a in (asked_s, asked_l)]
    return pl.pallas_call(
        attend_kernel,
        out_shape=shapes,
        in_specs=[vmem] * (2 + len(memories)),
        out_specs=[vmem, vmem],
        scratch_shapes=[pltpu.VMEM(memories[0].shape, jnp.bfloat16)],
        name="attend",
        cost_estimate=pl.CostEstimate(
            flops=2 * 6 * 2 * rows * rows * 4 * LANES,
            bytes_accessed=2 << 20,
            transcendentals=6 * rows * rows * 4,
        ),
        compiler_params=pltpu.CompilerParams(vmem_limit_bytes=16 << 20),
    )(asked_s, asked_l, *memories)


def pick_kernel(inner, outer, picked):
    at_inner = is_inner()

    @pl.when(at_inner)
    def _():
        picked[...] = inner[...]

    @pl.when(jnp.logical_not(at_inner))
    def _():
        picked[...] = outer[...]


def pick(inner, outer):
    vmem = pl.BlockSpec(memory_space=pltpu.VMEM)
    return pl.pallas_call(
        pick_kernel,
        out_shape=jax.ShapeDtypeStruct(inner.shape, inner.dtype),
        in_specs=[vmem, vmem],
        out_specs=vmem,
        name="pick",
        cost_estimate=pl.CostEstimate(flops=1000000, bytes_accessed=1 << 19, transcendentals=0),
        compiler_params=pltpu.CompilerParams(vmem_limit_bytes=2 << 20),
    )(inner, outer)


def expert_kernel(*refs):
    pieces, (blend, gate, up, down) = refs[:4], refs[4:8]
    kept, other, given, rows, active = refs[8:]
    local = pieces[0].shape[0]
    for place, piece in enumerate(pieces):
        rows[place * local : (place + 1) * local, :] = piece[...]
    width = gate.shape[2]
    columns = blend[...].T
    expert = lax.broadcasted_iota(jnp.int32, columns.shape, 1)
    first_expert = lax.axis_index("sp") * gate.shape[0]
    for place in range(gate.shape[0]):
        chosen = jnp.where(expert == first_expert + place, columns, 0.0)
        mixing = jnp.sum(chosen, axis=1, keepdims=True)
        gate_out = jnp.dot(rows[...], gate[place], preferred_element_type=jnp.float32)
        up_out = jnp.dot(rows[...], up[place], preferred_element_type=jnp.float32)
        result = gate_out / (1.0 + jnp.exp(-gate_out)) * up_out * mixing
        active[:, place * width : (place + 1) * width] = result.astype(jnp.bfloat16)
    step = 512
    for first in range(0, down.shape[1], step):
        columns = slice(first, first + step)
        out = jnp.dot(active[...], down[:, columns], preferred_element_type=jnp.float32)
        out = out.astype(jnp.bfloat16)
        kept[:, columns] = out[:local]
        other[:, columns] = out[local : 2 * local]
        given[:, columns] = out[2 * local :]


def run_experts(pieces, mixing, gate, up, down):
    local, wide = pieces[0].shape
    vmem = pl.BlockSpec(memory_space=pltpu.VMEM)
    hidden = gate.shape[0] * gate.shape[2]
    shapes = [jax.ShapeDtypeStruct((n, wide), jnp.bfloat16) for n in (local, local, 2 * local)]
    return pl.pallas_call(
        expert_kernel,
        out_shape=shapes,
        in_specs=[vmem] * 8,
        out_specs=[vmem] * 3,
        scratch_shapes=[
            pltpu.VMEM((4 * local, wide), jnp.bfloat16),
            pltpu.VMEM((4 * local, hidden), jnp.bfloat16),
        ],
        name="expert",
        cost_estimate=pl.CostEstimate(
            flops=6 * 4 * local * wide * hidden, bytes_accessed=4 << 20, transcendentals=0
        ),
        compiler_params=pltpu.CompilerParams(vmem_limit_bytes=16 << 20),
    )(*pieces, mixing, gate, up, down)


def gather_plan(
    queries_small,
    keys_small,
    values_small,
    queries_large,
    keys_large,
    values_large,
    query_gain_small,
    key_gain_small,
    query_gain_large,
    key_gain_large,
    residual_in,
    out_weight_small,
    out_weight_large,
    norm_gain,
    routes,
    route_scores,
    expert_gate,
    expert_up,
    expert_down,
):
    token_rows = queries_small.shape[0]
    local_rows = routes.shape[0]
    sp_count = lax.axis_size("sp")
    sp_index = lax.axis_index("sp")
    tp_index = lax.axis_index("tp")
    local_experts = expert_gate.shape[0]
    steps = list(range(sp_count))
    offset = sp_index * token_rows
    tables_small = grid_tables(offset, token_rows, HS_SMALL)
    tables_large = grid_tables(offset, token_rows, HS_LARGE)
    memory = make_memory(
        keys_small,
        values_small,
        keys_large,
        values_large,
        key_gain_small,
        key_gain_large,
        sp_count * token_rows // GRID_W,
    )
    second = meet(memory, 2)
    inner = inner_meet(memory)
    memories = [memory, meet(memory, 1), second, inner, meet(second, 1)]

    shares = route_scores / jnp.sum(route_scores, axis=1, keepdims=True)
    experts = jnp.arange(local_experts * sp_count, dtype=jnp.int32)
    named = (routes[:, :, None] == experts).astype(jnp.float32)
    mixing = jnp.sum(named * shares[:, :, None], axis=1).T
    mixing = gather_near(mixing, "tp", along=1)
    mixings = [mixing] + [meet(mixing, step) for step in steps[1:]]
    order = near_order("tp")

    def reorder(rows):
        return jnp.concatenate(
            [
                lax.dynamic_slice_in_dim(rows, (tp_index ^ place) * local_rows, local_rows, 0)
                for place in order
            ],
            axis=0,
        )

    asked_small = reorder(
        normed_turn(
            queries_small.reshape(token_rows, -1, HS_SMALL), query_gain_small, tables_small
        ).reshape(token_rows, -1)
    )
    asked_large = reorder(
        normed_turn(
            queries_large.reshape(token_rows, -1, HS_LARGE), query_gain_large, tables_large
        ).reshape(token_rows, -1)
    )
    heard_small, heard_large = attend_all(asked_small, asked_large, memories)

    def project(first, last):
        return (
            jnp.dot(
                heard_small[first:last], out_weight_small, preferred_element_type=jnp.float32
            )
            + jnp.dot(
                heard_large[first:last], out_weight_large, preferred_element_type=jnp.float32
            )
        ).astype(jnp.bfloat16)

    attended = add_near(project, token_rows)
    attended = (residual_in.astype(jnp.float32) + attended).astype(jnp.bfloat16)
    widened = attended.astype(jnp.float32)
    normed = (
        widened
        * lax.rsqrt(jnp.mean(widened * widened, axis=-1, keepdims=True) + norm_eps)
        * norm_gain
    ).astype(jnp.bfloat16)

    arrivals = [normed, meet(normed, 1), meet(normed, 2)]
    inner = inner_meet(normed)
    outer = meet(arrivals[2], 1)
    arrivals.append(pick(inner, outer))
    down = expert_down.reshape(-1, expert_down.shape[2])
    total = attended.astype(jnp.float32)
    near, far = flips("tp")
    for step in steps:
        own = arrivals[step]
        beside = swap(own, "tp", far)
        pieces = [own, beside]
        pieces += [swap(own, "tp", near), swap(beside, "tp", near)]
        kept, other, given = run_experts(pieces, mixings[step], expert_gate, expert_up, down)
        arrived = swap(given, "tp", near).astype(jnp.float32)
        other = (other.astype(jnp.float32) + arrived[local_rows:]).astype(jnp.bfloat16)
        crossed = swap(other, "tp", far).astype(jnp.float32)
        summed = kept.astype(jnp.float32) + arrived[:local_rows] + crossed
        if step:
            summed = summed.astype(jnp.bfloat16)
        if step:
            summed = meet(summed, step)
        total = total + summed.astype(jnp.float32)
    return total.astype(jnp.bfloat16)


def on_device(*arrays):
    routes, expert_gate = arrays[14], arrays[16]
    devices = lax.axis_size("sp") * lax.axis_size("tp")
    tokens = routes.shape[0] * devices
    expert_count = expert_gate.shape[0] * lax.axis_size("sp")
    capacity = max(2, (2 * routes.size + expert_count - 1) // expert_count)
    slots = devices * expert_gate.shape[0] * capacity
    tp_size = lax.axis_size("tp")
    widths = [array.shape[1] for array in arrays[:6]]
    fits = widths == [256, 128, 128, 256, 128, 128] and arrays[0].shape[0] % GRID_W == 0
    if tokens <= slots and tp_size == 4 and lax.axis_size("sp") == 4 and fits:
        return gather_plan(*arrays)
    return dispatch_plan(*arrays)


def solution(mesh):
    in_specs = (
        P(("grp", "sp"), "tp"),
        P(("grp", "sp"), "tp"),
        P(("grp", "sp"), "tp"),
        P(("grp", "sp"), "tp"),
        P(("grp", "sp"), "tp"),
        P(("grp", "sp"), "tp"),
        P("grp"),
        P("grp"),
        P("grp"),
        P("grp"),
        P(("grp", "sp", "tp"), None),
        P("tp", None),
        P("tp", None),
        P(),
        P(("grp", "sp", "tp"), None),
        P(("grp", "sp", "tp"), None),
        P("sp", None, "tp"),
        P("sp", None, "tp"),
        P("sp", "tp", None),
    )
    out_specs = P(("grp", "sp", "tp"), None)
    return jax.shard_map(
        on_device, mesh=mesh, in_specs=in_specs, out_specs=out_specs, check_vma=False
    )
```
